32 devices in a mesh: fs: 8 (over z, core), tp: 4 (over y, x).
Axes of the slice: x: 2, y: 2, z: 4, core: 2. Of those that a mesh axis runs over, the one named last changes fastest.
Arguments:
- saved_input: bfloat16 [6144, 2048], P('fs'), may hold values from -6 to 6
- query_cot: bfloat16 [6144, 2048], P('fs', 'tp'), may hold values from -120 to 120
- head_out: bfloat16 [6144, 2048], P('fs', 'tp'), may hold values from -120 to 120
- output_cot: bfloat16 [6144, 2048], P('fs'), may hold values from -6 to 6
- basis_q: bfloat16 [2048, 128], replicated, may hold values from -0.125 to 0.125
- basis_o: bfloat16 [2048, 128], replicated, may hold values from -0.125 to 0.125
- weight_q: float32 [2048, 2048], P('fs', 'tp'), may hold values from -0.125 to 0.125
- weight_o: float32 [2048, 2048], P('tp', 'fs'), may hold values from -0.125 to 0.125
- first_q: float32 [128, 2048], P(None, 'tp'), may hold values from -2 to 2
- second_q: float32 [128, 2048], P(None, 'tp'), may hold values from 0.01 to 1
- first_o: float32 [2048, 128], P('tp'), may hold values from -2 to 2
- second_o: float32 [2048, 128], P('tp'), may hold values from 0.01 to 1
Outputs:
- step_q: float32 [2048, 2048], P('fs', 'tp')
- step_o: float32 [2048, 2048], P('tp', 'fs')
- new_weight_q: float32 [2048, 2048], P('fs', 'tp')
- new_weight_o: float32 [2048, 2048], P('tp', 'fs')
- copy_q: bfloat16 [2048, 2048], P(None, 'tp')
- copy_o: bfloat16 [2048, 2048], P('tp')
- moment_q: float32 [128, 2048], P(None, 'tp')
- square_q: float32 [128, 2048], P(None, 'tp')
- moment_o: float32 [2048, 128], P('tp')
- square_o: float32 [2048, 128], P('tp')
The draws below stay inside these ranges and needn't reach their ends.
All inputs are finite; a program needn't handle non-finite values.
Results may differ from the reference program's by a relative error of at most 0.0035.
Values may be sent and summed in bfloat16 or wider, within the bound.
A program may use at most 64 MiB of HBM per device.

```python
import math
import jax
import jax.numpy as jnp
from jax import lax

D = 2048
HEADS = 16
HEAD = 128
RANK = 128
TOKENS = 6144
QDIM = 2048


def scaled_columns(key, salt):
    key = jax.random.fold_in(key, salt)
    drawn_key, column_key = jax.random.split(key, 2)
    full_width = HEADS * HEAD
    head_number = (jnp.arange(full_width) // HEAD).astype(jnp.float32)
    head_rise = 3.0 ** (head_number / max(HEADS - 1, 1))
    column_spread = 10.0 ** jax.random.uniform(column_key, (full_width,), jnp.float32)
    drawn_draw = jnp.clip(jax.random.normal(drawn_key, (TOKENS, full_width), jnp.float32), -4.0, 4.0)
    return (drawn_draw * head_rise * column_spread).astype(jnp.bfloat16)


def draw_query_cot(key, part):
    return scaled_columns(key, 11)


def draw_head_out(key, part):
    return scaled_columns(key, 23)


def strengthened(values, rng, source, target, shards_of, factor):
    def block_of(position):
        return (jnp.arange(values.shape[position]) // (values.shape[position] // shards_of)).reshape((-1,) + (1,) * (values.ndim - 1 - position))

    near = jax.random.permutation(rng, shards_of)[block_of(target)]
    other_side = (block_of(target) + shards_of // 2) % shards_of
    return jnp.where((block_of(source) == near) | (block_of(source) == other_side), factor * values, values)


def level_of(rng, shape, shards, least, top_value):
    def one(dim, parts):
        draws = jax.random.uniform(jax.random.fold_in(jax.random.fold_in(rng, 6), dim), (parts,), jnp.float32, least / len(shards), top_value / len(shards))
        return jnp.repeat(jnp.exp(draws), shape[dim] // parts).reshape((-1,) + (1,) * (len(shape) - dim - 1))

    level = one(*shards[0])
    for cut in shards[1:]:
        level = level * one(*cut)
    return level


def centred(stream_key, extent, width, most, cuts=(), held_as=jnp.bfloat16):
    drawn = width * jax.random.normal(stream_key, extent, jnp.float32)
    if cuts:
        drawn = drawn * level_of(stream_key, extent, cuts, -0.22, 0.18)
    return jnp.clip(drawn, -most, most).astype(held_as)


def noise_with(key, extent, scale, bound, cuts, heavy, kind=jnp.bfloat16):
    entries = scale * jax.random.normal(key, extent, jnp.float32)
    if cuts:
        entries = entries * level_of(key, extent, cuts, -0.22, 0.18)
    return jnp.clip(strengthened(entries, jax.random.fold_in(key, 3), *heavy), -bound, bound).astype(kind)


def setup_inputs(seed: int = 0) -> dict:
    arg_keys = jax.random.split(jax.random.key(seed), 13)
    return {
        "saved_input": noise_with(arg_keys[0], (TOKENS, D), 1.0, 6.0, ((0, 8),), (0, 1, 8, 2.0)),
        "query_cot": draw_query_cot(jax.random.fold_in(arg_keys[12], 71), 0),
        "head_out": draw_head_out(jax.random.fold_in(arg_keys[12], 71), 0),
        "output_cot": noise_with(arg_keys[3], (TOKENS, D), 1.0, 6.0, ((0, 8),), (0, 1, 8, 2.0)),
        "basis_q": centred(arg_keys[4], (D, RANK), D ** -0.5, 0.125),
        "basis_o": centred(arg_keys[5], (D, RANK), D ** -0.5, 0.125),
        "weight_q": centred(arg_keys[6], (D, QDIM), D ** -0.5, 0.125, ((0, 8), (1, 4)), jnp.float32),
        "weight_o": centred(arg_keys[7], (QDIM, D), QDIM ** -0.5, 0.125, ((0, 4), (1, 8)), jnp.float32),
        "first_q": centred(arg_keys[8], (RANK, QDIM), 0.3, 2.0, ((1, 4),), jnp.float32),
        "second_q": jnp.clip(jnp.exp(math.log(1.0) - 4.6051702 * jax.random.uniform(arg_keys[9], (RANK, QDIM), jnp.float32) ** level_of(arg_keys[9], (RANK, QDIM), ((1, 4),), -0.2, 0.2)), 0.01, 1.0),
        "first_o": centred(arg_keys[10], (QDIM, RANK), 0.3, 2.0, ((0, 4),), jnp.float32),
        "second_o": jnp.clip(jnp.exp(math.log(1.0) - 4.6051702 * jax.random.uniform(arg_keys[11], (QDIM, RANK), jnp.float32) ** level_of(arg_keys[11], (QDIM, RANK), ((0, 4),), -0.2, 0.2)), 0.01, 1.0),
    }


BETA_FIRST = 0.9
BETA_SECOND = 0.95
ADAM_EPS = 1e-08
NORM_EPS = 1e-06
CLIP_RMS = 1.0
LEARN_RATE = 0.01

def reference(saved_input, query_cot, head_out, output_cot, basis_q, basis_o, weight_q, weight_o, first_q, second_q, first_o, second_o):
    highest = lax.Precision.HIGHEST
    grad_q = jnp.dot(saved_input.T, query_cot, preferred_element_type=jnp.float32)
    grad_o = jnp.dot(head_out.T, output_cot, preferred_element_type=jnp.float32)
    low_q = jnp.dot(basis_q.astype(jnp.float32).T, grad_q, precision=highest)
    low_o = jnp.dot(grad_o, basis_o.astype(jnp.float32), precision=highest)
    square_total = jnp.sum(low_q * low_q) + jnp.sum(low_o * low_o)
    rms_value = jnp.sqrt(square_total / (2 * RANK * HEADS * HEAD) + NORM_EPS)
    factor = jnp.minimum(1.0, CLIP_RMS / rms_value)
    moment_q = BETA_FIRST * first_q + (1.0 - BETA_FIRST) * factor * low_q
    square_q = BETA_SECOND * second_q + (1.0 - BETA_SECOND) * (factor * low_q) ** 2
    moment_o = BETA_FIRST * first_o + (1.0 - BETA_FIRST) * factor * low_o
    square_o = BETA_SECOND * second_o + (1.0 - BETA_SECOND) * (factor * low_o) ** 2
    dir_q = moment_q / (jnp.sqrt(square_q) + ADAM_EPS)
    dir_o = moment_o / (jnp.sqrt(square_o) + ADAM_EPS)
    step_q = jnp.dot(basis_q.astype(jnp.float32), dir_q, precision=highest)
    step_o = jnp.dot(dir_o, basis_o.astype(jnp.float32).T, precision=highest)
    new_weight_q = weight_q - LEARN_RATE * step_q
    new_weight_o = weight_o - LEARN_RATE * step_o
    return (step_q, step_o, new_weight_q, new_weight_o, new_weight_q.astype(jnp.bfloat16), new_weight_o.astype(jnp.bfloat16), moment_q, square_q, moment_o, square_o)
```

```python
import functools

import jax
import jax.numpy as jnp
from jax import lax
from jax.experimental import pallas as pl
from jax.experimental.pallas import tpu as pltpu
from jax.sharding import PartitionSpec as P

MESH = pl.DeviceIdType.MESH
BETA_FIRST = 0.9
BETA_SECOND = 0.95
ADAM_EPS = 1e-08
NORM_EPS = 1e-06
CLIP_RMS = 1.0
LEARN_RATE = 0.01
CORES = 2
SCALE = 2.0**33


def split(value):
    upper = value.astype(jnp.bfloat16)
    lower = (value - upper.astype(jnp.float32)).astype(jnp.bfloat16)
    return upper, lower


def encode(weight):
    scaled = weight * SCALE
    square = scaled * scaled
    fourth = square * square
    return jnp.where(weight < 0, -fourth, fourth).astype(jnp.bfloat16)


def decode(code):
    value = code.astype(jnp.float32)
    root = lax.rsqrt(lax.rsqrt(jnp.abs(value))) * (1.0 / SCALE)
    return jnp.where(value < 0, -root, root)


def exchange(
    chips, columns, tile,
    x_hbm, qc_hbm, ho_hbm, oc_hbm, bq_hbm, bo_hbm, wq_hbm, wo_hbm,
    gq, go, low, total,
    xv, qcv, hov, ocv, bqv, bov, part, sib, acc, rs, sums,
    load, load_w, w_send, w_recv, ws_send, ws_recv,
    sib_sem, rs_send, rs_recv, ag_send, ag_recv, as_send, as_recv, tp_send, tp_recv,
):
    me = lax.axis_index("fs")
    tp = lax.axis_index("tp")
    z = me // CORES
    c = lax.rem(me, CORES)
    sibling = me + 1 - 2 * c
    tiles = xv.shape[0] // tile
    piece = acc.shape[1]
    gathered = (gq, go)

    own = [
        pltpu.make_async_copy(wq_hbm, gq.at[me], load_w.at[0]),
        pltpu.make_async_copy(wo_hbm, go.at[me], load_w.at[1]),
    ]
    for copy in own:
        copy.start()
    whole = ((bq_hbm, bqv), (bo_hbm, bov))
    cut = ((x_hbm, xv), (qc_hbm, qcv), (oc_hbm, ocv), (ho_hbm, hov))

    def load_of(k, t):
        source, target = cut[k]
        rows = pl.ds(t * tile, tile)
        return pltpu.make_async_copy(source.at[rows], target.at[rows], load.at[k, t])

    bases = [pltpu.make_async_copy(a, b, load_w.at[2 + i]) for i, (a, b) in enumerate(whole)]
    bases[0].start()
    for k in (0, 1):
        for t in range(tiles):
            load_of(k, t).start()
    bases[1].start()
    for k in (2, 3):
        for t in range(tiles):
            load_of(k, t).start()

    barrier = pltpu.get_barrier_semaphore()
    pl.semaphore_signal(barrier, inc=1, device_id={"fs": sibling}, device_id_type=MESH)
    for d in range(1, chips):
        other = lax.rem(z + d, chips) * CORES + c
        pl.semaphore_signal(barrier, inc=1, device_id={"fs": other}, device_id_type=MESH)
    for d in range(1, columns):
        other = lax.rem(tp + d, columns)
        pl.semaphore_signal(barrier, inc=1, device_id={"tp": other}, device_id_type=MESH)
    pl.semaphore_wait(barrier, 1 + chips - 1 + columns - 1)

    def along(m, b, k, s, target):
        slot = gathered[m].at[b * CORES + c]
        return pltpu.make_async_remote_copy(
            src_ref=slot, dst_ref=slot, send_sem=w_send.at[m, k, s], recv_sem=w_recv.at[m, b],
            device_id={"fs": target}, device_id_type=MESH,
        )

    def across(m, b, core):
        slot = gathered[m].at[b * CORES + core]
        return pltpu.make_async_remote_copy(
            src_ref=slot, dst_ref=slot, send_sem=ws_send.at[m, b], recv_sem=ws_recv.at[m, b],
            device_id={"fs": sibling}, device_id_type=MESH,
        )

    def relay(s, m, first=False):
        for k, sign in ((0, 1), (1, -1)):
            b = z - sign * s
            there = (b >= 0) & (b < chips)
            target = z + sign

            if not first:
                @pl.when(there)
                def _():
                    along(m, b, k, s, me).wait_recv()

            @pl.when(there & (target >= 0) & (target < chips))
            def _():
                along(m, b, k, s, target * CORES + c).start()

            if k == 0 or not first:
                @pl.when(there)
                def _():
                    across(m, b, c).start()

    for m in (0, 1):
        own[m].wait()
        relay(0, m, first=True)

    def multiply(m, basis, wide, narrow):
        def body(t, carry):
            load_of(2 * m, t).wait()
            rows = pl.ds(pl.multiple_of(t * tile, tile), tile)
            thin = jnp.dot(wide[rows, :], basis[...], preferred_element_type=jnp.float32)
            both = jnp.concatenate(split(thin), axis=1)
            load_of(2 * m + 1, t).wait()
            product = lax.dot_general(
                both, narrow[rows, :], (((0,), (0,)), ((), ())), preferred_element_type=jnp.float32
            )
            rank = product.shape[0] // 2
            value = product[:rank] + product[rank:]
            part[m] = value + jnp.where(t > 0, part[m], 0.0)
            return carry

        part[m] = jnp.zeros(part.shape[1:], part.dtype)
        lax.fori_loop(0, tiles, body, 0)

    bases[0].wait()
    multiply(0, bqv, xv, qcv)
    bases[1].wait()
    multiply(1, bov, ocv, hov)

    swap = pltpu.make_async_remote_copy(
        src_ref=part.at[1 - c], dst_ref=sib, send_sem=sib_sem.at[0], recv_sem=sib_sem.at[1],
        device_id={"fs": sibling}, device_id_type=MESH,
    )
    swap.start()
    swap.wait()
    value = part[c] + sib[...]
    for p in range(chips):
        acc[p] = value[p * piece : (p + 1) * piece]

    def scatter(d, source, target):
        return pltpu.make_async_remote_copy(
            src_ref=acc.at[target], dst_ref=rs.at[source], send_sem=rs_send.at[d], recv_sem=rs_recv.at[source],
            device_id={"fs": target * CORES + c}, device_id_type=MESH,
        )

    for d in range(1, chips):
        scatter(d, z, lax.rem(z + d, chips)).start()
    if chips > 1:
        relay(1, 0)
    rs[z] = acc[z]
    for d in range(1, chips):
        source = lax.rem(z + d, chips)
        scatter(d, source, z).wait_recv()
    reduced = rs[0]
    for p in range(1, chips):
        reduced = reduced + rs[p]
    low[c, z] = reduced

    def spread(d, source, target):
        return pltpu.make_async_remote_copy(
            src_ref=low.at[c, source], dst_ref=low.at[c, source], send_sem=ag_send.at[d], recv_sem=ag_recv.at[source],
            device_id={"fs": target * CORES + c}, device_id_type=MESH,
        )

    def hand(p, core):
        return pltpu.make_async_remote_copy(
            src_ref=low.at[core, p], dst_ref=low.at[core, p], send_sem=as_send.at[p], recv_sem=as_recv.at[p],
            device_id={"fs": sibling}, device_id_type=MESH,
        )

    for d in range(1, chips):
        spread(d, z, lax.rem(z + d, chips)).start()
    hand(z, c).start()
    if chips > 1:
        relay(1, 1)
    for d in range(1, chips):
        source = lax.rem(z + d, chips)
        spread(d, source, z).wait_recv()
        hand(source, c).start()
    for p in range(chips):
        hand(p, 1 - c).wait_recv()

    squares = jnp.zeros(acc.shape[1:], jnp.float32)
    for core in range(CORES):
        for p in range(chips):
            entry = low[core, p]
            squares = squares + entry * entry
    sums[tp] = jnp.broadcast_to(jnp.sum(squares, axis=(0, 1), keepdims=True), sums.shape[1:])

    def share(d, source, target):
        return pltpu.make_async_remote_copy(
            src_ref=sums.at[source], dst_ref=sums.at[source], send_sem=tp_send.at[d], recv_sem=tp_recv.at[source],
            device_id={"tp": target}, device_id_type=MESH,
        )

    for d in range(1, columns):
        share(d, tp, lax.rem(tp + d, columns)).start()
    for d in range(1, columns):
        share(d, lax.rem(tp + d, columns), tp).wait_recv()
    everything = sums[0]
    for p in range(1, columns):
        everything = everything + sums[p]
    total[...] = everything

    if chips > 2:
        @pl.loop(2, chips)
        def _(s):
            for m in (0, 1):
                relay(s, m)

    for m in (0, 1):
        for p in range(chips):
            across(m, p, 1 - c).wait_recv()
            across(m, p, c).wait_send()

        @pl.loop(0, chips)
        def _(s):
            for k, sign in ((0, 1), (1, -1)):
                b = z - sign * s
                target = z + sign

                @pl.when((b >= 0) & (b < chips) & (target >= 0) & (target < chips))
                def _():
                    along(m, b, k, s, target * CORES + c).wait_send()

    for d in range(1, chips):
        scatter(d, z, lax.rem(z + d, chips)).wait_send()
        spread(d, z, lax.rem(z + d, chips)).wait_send()
    for p in range(chips):
        hand(p, c).wait_send()
    for d in range(1, columns):
        share(d, tp, lax.rem(tp + d, columns)).wait_send()


def communicate(fs, columns, x, qc, ho, oc, bq, bo, wq, wo):
    chips = fs // CORES
    tokens, width = x.shape
    features = qc.shape[1]
    rank = bq.shape[1]
    piece = rank // chips
    tile = 256 if tokens % 256 == 0 else tokens
    dma = pltpu.SemaphoreType.DMA
    f32 = jnp.float32
    return pl.pallas_call(
        functools.partial(exchange, chips, columns, tile),
        out_shape=(
            jax.ShapeDtypeStruct((fs,) + wq.shape, wq.dtype),
            jax.ShapeDtypeStruct((fs,) + wo.shape, wo.dtype),
            jax.ShapeDtypeStruct((CORES, chips, piece, features), f32),
            jax.ShapeDtypeStruct((8, 128), f32),
        ),
        in_specs=[pl.BlockSpec(memory_space=pl.ANY)] * 8,
        out_specs=[pl.BlockSpec(memory_space=pltpu.VMEM)] * 4,
        scratch_shapes=[
            pltpu.VMEM(x.shape, x.dtype),
            pltpu.VMEM(qc.shape, qc.dtype),
            pltpu.VMEM(ho.shape, ho.dtype),
            pltpu.VMEM(oc.shape, oc.dtype),
            pltpu.VMEM(bq.shape, bq.dtype),
            pltpu.VMEM(bo.shape, bo.dtype),
            pltpu.VMEM((2, rank, features), f32),
            pltpu.VMEM((rank, features), f32),
            pltpu.VMEM((chips, piece, features), f32),
            pltpu.VMEM((chips, piece, features), f32),
            pltpu.VMEM((columns, 8, 128), f32),
            dma((4, tokens // tile)),
            dma((4,)),
            dma((2, 2, chips)),
            dma((2, chips)),
            dma((2, chips)),
            dma((2, chips)),
            dma((2,)),
            dma((chips,)),
            dma((chips,)),
            dma((chips,)),
            dma((chips,)),
            dma((chips,)),
            dma((chips,)),
            dma((columns,)),
            dma((columns,)),
        ],
        compiler_params=pltpu.CompilerParams(
            collective_id=0, has_side_effects=True, vmem_limit_bytes=48 * 1024 * 1024
        ),
        name="exchange",
    )(x, qc, ho, oc, bq, bo, wq, wo)


def shards(
    fs, columns,
    saved_input, query_cot, head_out, output_cot, basis_q, basis_o,
    weight_q, weight_o, first_q, second_q, first_o, second_o,
):
    f32 = jnp.float32
    rank = basis_q.shape[1]
    features = query_cot.shape[1]
    rows = weight_q.shape[0]
    send_q = encode(weight_q)
    send_o = encode(weight_o)
    all_q, all_o, low, total = communicate(
        fs, columns, saved_input, query_cot, head_out, output_cot, basis_q, basis_o, send_q, send_o
    )
    low_q = low[0].reshape(rank, features)
    low_o = low[1].reshape(rank, features).T
    rms_value = jnp.sqrt(total[0, 0] / (2 * rank * features * columns) + NORM_EPS)
    factor = jnp.minimum(1.0, CLIP_RMS / rms_value)
    moment_q = BETA_FIRST * first_q + (1.0 - BETA_FIRST) * factor * low_q
    square_q = BETA_SECOND * second_q + (1.0 - BETA_SECOND) * (factor * low_q) ** 2
    moment_o = BETA_FIRST * first_o + (1.0 - BETA_FIRST) * factor * low_o
    square_o = BETA_SECOND * second_o + (1.0 - BETA_SECOND) * (factor * low_o) ** 2
    dir_q = moment_q / (jnp.sqrt(square_q) + ADAM_EPS)
    dir_o = moment_o / (jnp.sqrt(square_o) + ADAM_EPS)
    upper_q, lower_q = split(dir_q)
    upper_o, lower_o = split(dir_o)

    def steps(bq, bo):
        q = jnp.dot(bq, upper_q, preferred_element_type=f32) + jnp.dot(bq, lower_q, preferred_element_type=f32)
        o = jnp.dot(upper_o, bo.T, preferred_element_type=f32) + jnp.dot(lower_o, bo.T, preferred_element_type=f32)
        return q, o

    offset = lax.axis_index("fs") * rows
    step_q, step_o = steps(
        lax.dynamic_slice_in_dim(basis_q, offset, rows, 0), lax.dynamic_slice_in_dim(basis_o, offset, rows, 0)
    )
    new_weight_q = weight_q - LEARN_RATE * step_q
    new_weight_o = weight_o - LEARN_RATE * step_o
    full_q, full_o = steps(basis_q, basis_o)
    old_q = decode(all_q.reshape(fs * rows, features))
    old_o = decode(all_o.transpose(1, 0, 2).reshape(features, fs * rows))
    copy_q = (old_q - LEARN_RATE * full_q).astype(jnp.bfloat16)
    copy_o = (old_o - LEARN_RATE * full_o).astype(jnp.bfloat16)
    return (
        step_q, step_o, new_weight_q, new_weight_o, copy_q, copy_o,
        moment_q, square_q, moment_o, square_o,
    )


def solution(mesh):
    return jax.shard_map(
        functools.partial(shards, mesh.shape["fs"], mesh.shape["tp"]),
        mesh=mesh,
        in_specs=(
            P("fs", None), P("fs", "tp"), P("fs", "tp"), P("fs", None), P(), P(),
            P("fs", "tp"), P("tp", "fs"), P(None, "tp"), P(None, "tp"), P("tp", None), P("tp", None),
        ),
        out_specs=(
            P("fs", "tp"), P("tp", "fs"), P("fs", "tp"), P("tp", "fs"), P(None, "tp"), P("tp", None),
            P(None, "tp"), P(None, "tp"), P("tp", None), P("tp", None),
        ),
        check_vma=False,
    )
```

```python
import functools

import jax
import jax.numpy as jnp
from jax import lax
from jax.experimental import pallas as pl
from jax.experimental.pallas import tpu as pltpu
from jax.sharding import PartitionSpec as P

MESH = pl.DeviceIdType.MESH
BETA_FIRST = 0.9
BETA_SECOND = 0.95
ADAM_EPS = 1e-08
NORM_EPS = 1e-06
CLIP_RMS = 1.0
LEARN_RATE = 0.01
CORES = 2
SCALE = 2.0**33


def split(value):
    upper = value.astype(jnp.bfloat16)
    lower = (value - upper.astype(jnp.float32)).astype(jnp.bfloat16)
    return upper, lower


def encode(weight):
    scaled = weight * SCALE
    square = scaled * scaled
    fourth = square * square
    return jnp.where(weight < 0, -fourth, fourth).astype(jnp.bfloat16)


def decode(code):
    value = code.astype(jnp.float32)
    root = lax.rsqrt(lax.rsqrt(jnp.abs(value))) * (1.0 / SCALE)
    return jnp.where(value < 0, -root, root)


def exchange(
    chips, columns, tile,
    x_hbm, qc_hbm, ho_hbm, oc_hbm, bq_hbm, bo_hbm, wq_hbm, wo_hbm,
    gq, go, low, total,
    xv, qcv, hov, ocv, bqv, bov, part, sib, acc, rs, sums,
    load, load_w, w_send, w_recv, ws_send, ws_recv,
    sib_sem, rs_send, rs_recv, ag_send, ag_recv, as_send, as_recv, tp_send, tp_recv,
):
    me = lax.axis_index("fs")
    tp = lax.axis_index("tp")
    z = me // CORES
    c = lax.rem(me, CORES)
    sibling = me + 1 - 2 * c
    tiles = xv.shape[0] // tile
    piece = acc.shape[1]
    gathered = (gq, go)

    own = [
        pltpu.make_async_copy(wq_hbm, gq.at[me], load_w.at[0]),
        pltpu.make_async_copy(wo_hbm, go.at[me], load_w.at[1]),
    ]
    for copy in own:
        copy.start()
    whole = ((bq_hbm, bqv), (bo_hbm, bov))
    cut = ((x_hbm, xv), (qc_hbm, qcv), (oc_hbm, ocv), (ho_hbm, hov))

    def load_of(k, t):
        source, target = cut[k]
        rows = pl.ds(t * tile, tile)
        return pltpu.make_async_copy(source.at[rows], target.at[rows], load.at[k, t])

    bases = [pltpu.make_async_copy(a, b, load_w.at[2 + i]) for i, (a, b) in enumerate(whole)]
    bases[0].start()
    for k in (0, 1):
        for t in range(tiles):
            load_of(k, t).start()
    bases[1].start()
    for k in (2, 3):
        for t in range(tiles):
            load_of(k, t).start()

    barrier = pltpu.get_barrier_semaphore()
    pl.semaphore_signal(barrier, inc=1, device_id={"fs": sibling}, device_id_type=MESH)
    for d in range(1, chips):
        other = lax.rem(z + d, chips) * CORES + c
        pl.semaphore_signal(barrier, inc=1, device_id={"fs": other}, device_id_type=MESH)
    for d in range(1, columns):
        other = lax.rem(tp + d, columns)
        pl.semaphore_signal(barrier, inc=1, device_id={"tp": other}, device_id_type=MESH)
    pl.semaphore_wait(barrier, 1 + chips - 1 + columns - 1)

    def along(m, b, k, s, target):
        slot = gathered[m].at[b * CORES + c]
        return pltpu.make_async_remote_copy(
            src_ref=slot, dst_ref=slot, send_sem=w_send.at[m, k, s], recv_sem=w_recv.at[m, b],
            device_id={"fs": target}, device_id_type=MESH,
        )

    def across(m, b, core):
        slot = gathered[m].at[b * CORES + core]
        return pltpu.make_async_remote_copy(
            src_ref=slot, dst_ref=slot, send_sem=ws_send.at[m, b], recv_sem=ws_recv.at[m, b],
            device_id={"fs": sibling}, device_id_type=MESH,
        )

    def relay(s, m, first=False):
        for k, sign in ((0, 1), (1, -1)):
            b = z - sign * s
            there = (b >= 0) & (b < chips)
            target = z + sign

            if not first:
                @pl.when(there)
                def _():
                    along(m, b, k, s, me).wait_recv()

            @pl.when(there & (target >= 0) & (target < chips))
            def _():
                along(m, b, k, s, target * CORES + c).start()

            if k == 0 or not first:
                @pl.when(there)
                def _():
                    across(m, b, c).start()

    for m in (0, 1):
        own[m].wait()
        relay(0, m, first=True)

    def multiply(m, basis, wide, narrow):
        def body(t, carry):
            load_of(2 * m, t).wait()
            rows = pl.ds(pl.multiple_of(t * tile, tile), tile)
            thin = jnp.dot(wide[rows, :], basis[...], preferred_element_type=jnp.float32)
            both = jnp.concatenate(split(thin), axis=1)
            load_of(2 * m + 1, t).wait()
            product = lax.dot_general(
                both, narrow[rows, :], (((0,), (0,)), ((), ())), preferred_element_type=jnp.float32
            )
            rank = product.shape[0] // 2
            value = product[:rank] + product[rank:]
            part[m] = value + jnp.where(t > 0, part[m], 0.0)
            return carry

        part[m] = jnp.zeros(part.shape[1:], part.dtype)
        lax.fori_loop(0, tiles, body, 0)

    bases[0].wait()
    multiply(0, bqv, xv, qcv)
    bases[1].wait()
    multiply(1, bov, ocv, hov)

    swap = pltpu.make_async_remote_copy(
        src_ref=part.at[1 - c], dst_ref=sib, send_sem=sib_sem.at[0], recv_sem=sib_sem.at[1],
        device_id={"fs": sibling}, device_id_type=MESH,
    )
    swap.start()
    swap.wait()
    value = part[c] + sib[...]
    for p in range(chips):
        acc[p] = value[p * piece : (p + 1) * piece]

    def scatter(d, source, target):
        return pltpu.make_async_remote_copy(
            src_ref=acc.at[target], dst_ref=rs.at[source], send_sem=rs_send.at[d], recv_sem=rs_recv.at[source],
            device_id={"fs": target * CORES + c}, device_id_type=MESH,
        )

    for d in range(1, chips):
        scatter(d, z, lax.rem(z + d, chips)).start()
    if chips > 1:
        relay(1, 0)
    rs[z] = acc[z]
    for d in range(1, chips):
        source = lax.rem(z + d, chips)
        scatter(d, source, z).wait_recv()
    reduced = rs[0]
    for p in range(1, chips):
        reduced = reduced + rs[p]
    low[c, z] = reduced

    def spread(d, source, target):
        return pltpu.make_async_remote_copy(
            src_ref=low.at[c, source], dst_ref=low.at[c, source], send_sem=ag_send.at[d], recv_sem=ag_recv.at[source],
            device_id={"fs": target * CORES + c}, device_id_type=MESH,
        )

    def hand(p, core):
        return pltpu.make_async_remote_copy(
            src_ref=low.at[core, p], dst_ref=low.at[core, p], send_sem=as_send.at[p], recv_sem=as_recv.at[p],
            device_id={"fs": sibling}, device_id_type=MESH,
        )

    for d in range(1, chips):
        spread(d, z, lax.rem(z + d, chips)).start()
    hand(z, c).start()
    if chips > 1:
        relay(1, 1)
    for d in range(1, chips):
        source = lax.rem(z + d, chips)
        spread(d, source, z).wait_recv()
        hand(source, c).start()
    for p in range(chips):
        hand(p, 1 - c).wait_recv()

    squares = jnp.zeros(acc.shape[1:], jnp.float32)
    for core in range(CORES):
        for p in range(chips):
            entry = low[core, p]
            squares = squares + entry * entry
    sums[tp] = jnp.broadcast_to(jnp.sum(squares, axis=(0, 1), keepdims=True), sums.shape[1:])

    def share(d, source, target):
        return pltpu.make_async_remote_copy(
            src_ref=sums.at[source], dst_ref=sums.at[source], send_sem=tp_send.at[d], recv_sem=tp_recv.at[source],
            device_id={"tp": target}, device_id_type=MESH,
        )

    for d in range(1, columns):
        share(d, tp, lax.rem(tp + d, columns)).start()
    for d in range(1, columns):
        share(d, lax.rem(tp + d, columns), tp).wait_recv()
    everything = sums[0]
    for p in range(1, columns):
        everything = everything + sums[p]
    total[...] = everything

    if chips > 2:
        @pl.loop(2, chips)
        def _(s):
            for m in (0, 1):
                relay(s, m)

    for m in (0, 1):
        for p in range(chips):
            across(m, p, 1 - c).wait_recv()
            across(m, p, c).wait_send()

        @pl.loop(0, chips)
        def _(s):
            for k, sign in ((0, 1), (1, -1)):
                b = z - sign * s
                target = z + sign

                @pl.when((b >= 0) & (b < chips) & (target >= 0) & (target < chips))
                def _():
                    along(m, b, k, s, target * CORES + c).wait_send()

    for d in range(1, chips):
        scatter(d, z, lax.rem(z + d, chips)).wait_send()
        spread(d, z, lax.rem(z + d, chips)).wait_send()
    for p in range(chips):
        hand(p, c).wait_send()
    for d in range(1, columns):
        share(d, tp, lax.rem(tp + d, columns)).wait_send()


def communicate(fs, columns, x, qc, ho, oc, bq, bo, wq, wo):
    chips = fs // CORES
    tokens, width = x.shape
    features = qc.shape[1]
    rank = bq.shape[1]
    piece = rank // chips
    tile = 256 if tokens % 256 == 0 else tokens
    dma = pltpu.SemaphoreType.DMA
    f32 = jnp.float32
    return pl.pallas_call(
        functools.partial(exchange, chips, columns, tile),
        out_shape=(
            jax.ShapeDtypeStruct((fs,) + wq.shape, wq.dtype),
            jax.ShapeDtypeStruct((fs,) + wo.shape, wo.dtype),
            jax.ShapeDtypeStruct((CORES, chips, piece, features), f32),
            jax.ShapeDtypeStruct((8, 128), f32),
        ),
        in_specs=[pl.BlockSpec(memory_space=pl.ANY)] * 8,
        out_specs=[pl.BlockSpec(memory_space=pltpu.VMEM)] * 4,
        scratch_shapes=[
            pltpu.VMEM(x.shape, x.dtype),
            pltpu.VMEM(qc.shape, qc.dtype),
            pltpu.VMEM(ho.shape, ho.dtype),
            pltpu.VMEM(oc.shape, oc.dtype),
            pltpu.VMEM(bq.shape, bq.dtype),
            pltpu.VMEM(bo.shape, bo.dtype),
            pltpu.VMEM((2, rank, features), f32),
            pltpu.VMEM((rank, features), f32),
            pltpu.VMEM((chips, piece, features), f32),
            pltpu.VMEM((chips, piece, features), f32),
            pltpu.VMEM((columns, 8, 128), f32),
            dma((4, tokens // tile)),
            dma((4,)),
            dma((2, 2, chips)),
            dma((2, chips)),
            dma((2, chips)),
            dma((2, chips)),
            dma((2,)),
            dma((chips,)),
            dma((chips,)),
            dma((chips,)),
            dma((chips,)),
            dma((chips,)),
            dma((chips,)),
            dma((columns,)),
            dma((columns,)),
        ],
        compiler_params=pltpu.CompilerParams(
            collective_id=0, has_side_effects=True, vmem_limit_bytes=48 * 1024 * 1024
        ),
        name="exchange",
    )(x, qc, ho, oc, bq, bo, wq, wo)


def adam(low, first, second, factor):
    scaled = factor * low
    moment = BETA_FIRST * first + (1.0 - BETA_FIRST) * scaled
    square = BETA_SECOND * second + (1.0 - BETA_SECOND) * (scaled * scaled)
    return moment, square, moment / (jnp.sqrt(square) + ADAM_EPS)


def finish(fs, count, *refs):
    gq, go, low, total, bq, bo, wq, wo, fq, sq, fo, so = refs[:12]
    outs, made, sem = refs[12:22], refs[22:32], refs[32]
    step_q, step_o, new_q, new_o, copy_q, copy_o, moment_q, square_q, moment_o, square_o = made
    f32 = jnp.float32
    me = lax.axis_index("fs")
    rows = wq.shape[0]
    features = wo.shape[0]
    started = []

    def write(i, part=None, index=0):
        source, target = made[i], outs[i]
        if part is not None:
            source, target = source.at[part], target.at[part]
        copy = pltpu.make_async_copy(source, target, sem.at[i, index])
        copy.start()
        started.append(copy)

    factor = jnp.minimum(1.0, CLIP_RMS / jnp.sqrt(total[0:1, 0:1] * (1.0 / count) + NORM_EPS))
    low_q = jnp.concatenate([low[0, p] for p in range(low.shape[1])], axis=0)
    moment_q[...], square_q[...], dir_q = adam(low_q, fq[...], sq[...], factor)
    write(6)
    write(7)
    low_o = jnp.concatenate([low[1, p] for p in range(low.shape[1])], axis=0).T
    moment_o[...], square_o[...], dir_o = adam(low_o, fo[...], so[...], factor)
    write(8)
    write(9)
    pair_q = jnp.concatenate(split(dir_q), axis=0)
    pair_o = jnp.concatenate(split(dir_o), axis=1)

    def make_q(part):
        basis = bq[part, :]
        return jnp.dot(jnp.concatenate([basis, basis], axis=1), pair_q, preferred_element_type=f32)

    def make_o(left, part):
        basis = bo[part, :]
        both = jnp.concatenate([basis, basis], axis=1)
        return lax.dot_general(left, both, (((1,), (1,)), ((), ())), preferred_element_type=f32)

    mine = pl.ds(pl.multiple_of(me * rows, rows), rows)
    step = make_q(mine)
    step_q[...] = step
    new_q[...] = wq[...] - LEARN_RATE * step
    write(0)
    write(2)
    step = make_o(pair_o, mine)
    step_o[...] = step
    new_o[...] = wo[...] - LEARN_RATE * step
    write(1)
    write(3)

    for j in range(fs):
        part = pl.ds(j * rows, rows)
        copy_q[part, :] = (decode(gq[j]) - LEARN_RATE * make_q(part)).astype(copy_q.dtype)
        write(4, part, j)
    tall = 128
    for r in range(features // tall):
        part = pl.ds(r * tall, tall)
        left = pair_o[r * tall : (r + 1) * tall]
        for j in range(fs):
            columns = pl.ds(j * rows, rows)
            value = decode(go[j, part, :]) - LEARN_RATE * make_o(left, columns)
            copy_o[part, columns] = value.astype(copy_o.dtype)
        write(5, part, r)
    for copy in started:
        copy.wait()


def update(fs, columns, gq, go, low, total, bq, bo, wq, wo, fq, sq, fo, so):
    f32 = jnp.float32
    rank, features = fq.shape
    rows = wq.shape[0]
    width = fs * rows
    outs = (
        (wq.shape, f32), (wo.shape, f32), (wq.shape, f32), (wo.shape, f32),
        ((width, features), jnp.bfloat16), ((features, width), jnp.bfloat16),
        (fq.shape, f32), (fq.shape, f32), (fo.shape, f32), (fo.shape, f32),
    )
    return pl.pallas_call(
        functools.partial(finish, fs, 2 * rank * features * columns),
        out_shape=tuple(jax.ShapeDtypeStruct(*out) for out in outs),
        in_specs=[pl.BlockSpec(memory_space=pltpu.VMEM)] * 12,
        out_specs=[pl.BlockSpec(memory_space=pl.ANY)] * 10,
        scratch_shapes=[pltpu.VMEM(*out) for out in outs] + [pltpu.SemaphoreType.DMA((10, max(fs, features // 128)))],
        compiler_params=pltpu.CompilerParams(vmem_limit_bytes=48 * 1024 * 1024),
        name="update",
    )(gq, go, low, total, bq, bo, wq, wo, fq, sq, fo, so)


def shards(
    fs, columns,
    saved_input, query_cot, head_out, output_cot, basis_q, basis_o,
    weight_q, weight_o, first_q, second_q, first_o, second_o,
):
    send_q = encode(weight_q)
    send_o = encode(weight_o)
    all_q, all_o, low, total = communicate(
        fs, columns, saved_input, query_cot, head_out, output_cot, basis_q, basis_o, send_q, send_o
    )
    return update(
        fs, columns, all_q, all_o, low, total, basis_q, basis_o,
        weight_q, weight_o, first_q, second_q, first_o, second_o,
    )


def solution(mesh):
    return jax.shard_map(
        functools.partial(shards, mesh.shape["fs"], mesh.shape["tp"]),
        mesh=mesh,
        in_specs=(
            P("fs", None), P("fs", "tp"), P("fs", "tp"), P("fs", None), P(), P(),
            P("fs", "tp"), P("tp", "fs"), P(None, "tp"), P(None, "tp"), P("tp", None), P("tp", None),
        ),
        out_specs=(
            P("fs", "tp"), P("tp", "fs"), P("fs", "tp"), P("tp", "fs"), P(None, "tp"), P("tp", None),
            P(None, "tp"), P(None, "tp"), P("tp", None), P("tp", None),
        ),
        check_vma=False,
    )
```

```python
import functools

import jax
import jax.numpy as jnp
from jax import lax
from jax.experimental import pallas as pl
from jax.experimental.pallas import tpu as pltpu
from jax.sharding import PartitionSpec as P

MESH = pl.DeviceIdType.MESH
BETA_FIRST = 0.9
BETA_SECOND = 0.95
ADAM_EPS = 1e-08
NORM_EPS = 1e-06
CLIP_RMS = 1.0
LEARN_RATE = 0.01
CORES = 2
SCALE = 2.0**33


def split(value):
    upper = value.astype(jnp.bfloat16)
    lower = (value - upper.astype(jnp.float32)).astype(jnp.bfloat16)
    return upper, lower


def encode(weight):
    scaled = weight * SCALE
    square = scaled * scaled
    fourth = square * square
    return jnp.where(weight < 0, -fourth, fourth).astype(jnp.bfloat16)


def decode(code):
    value = code.astype(jnp.float32)
    root = lax.rsqrt(lax.rsqrt(jnp.abs(value))) * (1.0 / SCALE)
    return jnp.where(value < 0, -root, root)


def exchange(
    chips, columns, tile,
    x_hbm, qc_hbm, ho_hbm, oc_hbm, bq_hbm, bo_hbm, wq_hbm, wo_hbm,
    gq, go, low, total,
    xv, qcv, hov, ocv, bqv, bov, wqv, wov, part, sib, acc, rs, sums,
    load, load_w, w_send, w_recv, ws_send, ws_recv,
    sib_sem, rs_send, rs_recv, ag_send, ag_recv, as_send, as_recv, tp_send, tp_recv,
):
    me = lax.axis_index("fs")
    tp = lax.axis_index("tp")
    z = me // CORES
    c = lax.rem(me, CORES)
    sibling = me + 1 - 2 * c
    tiles = xv.shape[0] // tile
    piece = acc.shape[1]
    gathered = (gq, go)

    own = [
        pltpu.make_async_copy(wq_hbm, wqv, load_w.at[0]),
        pltpu.make_async_copy(wo_hbm, wov, load_w.at[1]),
    ]
    for copy in own:
        copy.start()
    whole = ((bq_hbm, bqv), (bo_hbm, bov))
    cut = ((x_hbm, xv), (qc_hbm, qcv), (oc_hbm, ocv), (ho_hbm, hov))

    def load_of(k, t):
        source, target = cut[k]
        rows = pl.ds(t * tile, tile)
        return pltpu.make_async_copy(source.at[rows], target.at[rows], load.at[k, t])

    bases = [pltpu.make_async_copy(a, b, load_w.at[2 + i]) for i, (a, b) in enumerate(whole)]
    bases[0].start()
    for k in (0, 1):
        for t in range(tiles):
            load_of(k, t).start()
    bases[1].start()
    for k in (2, 3):
        for t in range(tiles):
            load_of(k, t).start()

    barrier = pltpu.get_barrier_semaphore()
    pl.semaphore_signal(barrier, inc=1, device_id={"fs": sibling}, device_id_type=MESH)
    for d in range(1, chips):
        other = lax.rem(z + d, chips) * CORES + c
        pl.semaphore_signal(barrier, inc=1, device_id={"fs": other}, device_id_type=MESH)
    for d in range(1, columns):
        other = lax.rem(tp + d, columns)
        pl.semaphore_signal(barrier, inc=1, device_id={"tp": other}, device_id_type=MESH)
    for m, weight in enumerate((wqv, wov)):
        own[m].wait()
        gathered[m][me] = encode(weight[...])
    pl.semaphore_wait(barrier, 1 + chips - 1 + columns - 1)

    def along(m, b, k, s, target):
        slot = gathered[m].at[b * CORES + c]
        return pltpu.make_async_remote_copy(
            src_ref=slot, dst_ref=slot, send_sem=w_send.at[m, k, s], recv_sem=w_recv.at[m, b],
            device_id={"fs": target}, device_id_type=MESH,
        )

    def across(m, b, core):
        slot = gathered[m].at[b * CORES + core]
        return pltpu.make_async_remote_copy(
            src_ref=slot, dst_ref=slot, send_sem=ws_send.at[m, b], recv_sem=ws_recv.at[m, b],
            device_id={"fs": sibling}, device_id_type=MESH,
        )

    def relay(s, m, first=False):
        for k, sign in ((0, 1), (1, -1)):
            b = z - sign * s
            there = (b >= 0) & (b < chips)
            target = z + sign

            if not first:
                @pl.when(there)
                def _():
                    along(m, b, k, s, me).wait_recv()

            @pl.when(there & (target >= 0) & (target < chips))
            def _():
                along(m, b, k, s, target * CORES + c).start()

            if k == 0 or not first:
                @pl.when(there)
                def _():
                    across(m, b, c).start()

    for m in (0, 1):
        relay(0, m, first=True)

    def multiply(m, basis, wide, narrow):
        def body(t, carry):
            load_of(2 * m, t).wait()
            rows = pl.ds(pl.multiple_of(t * tile, tile), tile)
            thin = jnp.dot(wide[rows, :], basis[...], preferred_element_type=jnp.float32)
            both = jnp.concatenate(split(thin), axis=1)
            load_of(2 * m + 1, t).wait()
            product = lax.dot_general(
                both, narrow[rows, :], (((0,), (0,)), ((), ())), preferred_element_type=jnp.float32
            )
            rank = product.shape[0] // 2
            value = product[:rank] + product[rank:]
            part[m] = value + jnp.where(t > 0, part[m], 0.0)
            return carry

        part[m] = jnp.zeros(part.shape[1:], part.dtype)
        lax.fori_loop(0, tiles, body, 0)

    bases[0].wait()
    multiply(0, bqv, xv, qcv)
    bases[1].wait()
    multiply(1, bov, ocv, hov)
    if chips > 1:
        relay(1, 0)

    swap = pltpu.make_async_remote_copy(
        src_ref=part.at[1 - c], dst_ref=sib, send_sem=sib_sem.at[0], recv_sem=sib_sem.at[1],
        device_id={"fs": sibling}, device_id_type=MESH,
    )
    swap.start()
    swap.wait()
    value = part[c] + sib[...]
    for p in range(chips):
        acc[p] = value[p * piece : (p + 1) * piece]

    def scatter(d, source, target):
        return pltpu.make_async_remote_copy(
            src_ref=acc.at[target], dst_ref=rs.at[source], send_sem=rs_send.at[d], recv_sem=rs_recv.at[source],
            device_id={"fs": target * CORES + c}, device_id_type=MESH,
        )

    for d in range(1, chips):
        scatter(d, z, lax.rem(z + d, chips)).start()
    if chips > 1:
        relay(1, 1)
    rs[z] = acc[z]
    for d in range(1, chips):
        source = lax.rem(z + d, chips)
        scatter(d, source, z).wait_recv()
    reduced = rs[0]
    for p in range(1, chips):
        reduced = reduced + rs[p]
    low[c, z] = reduced

    def spread(d, source, target):
        return pltpu.make_async_remote_copy(
            src_ref=low.at[c, source], dst_ref=low.at[c, source], send_sem=ag_send.at[d], recv_sem=ag_recv.at[source],
            device_id={"fs": target * CORES + c}, device_id_type=MESH,
        )

    def hand(p, core):
        return pltpu.make_async_remote_copy(
            src_ref=low.at[core, p], dst_ref=low.at[core, p], send_sem=as_send.at[p], recv_sem=as_recv.at[p],
            device_id={"fs": sibling}, device_id_type=MESH,
        )

    for d in range(1, chips):
        spread(d, z, lax.rem(z + d, chips)).start()
    hand(z, c).start()
    if chips > 2:
        relay(2, 0)
        relay(2, 1)
    for d in range(1, chips):
        source = lax.rem(z + d, chips)
        spread(d, source, z).wait_recv()
        hand(source, c).start()
    for p in range(chips):
        hand(p, 1 - c).wait_recv()

    squares = jnp.zeros(acc.shape[1:], jnp.float32)
    for core in range(CORES):
        for p in range(chips):
            entry = low[core, p]
            squares = squares + entry * entry
    sums[tp] = jnp.broadcast_to(jnp.sum(squares, axis=(0, 1), keepdims=True), sums.shape[1:])

    def share(d, source, target):
        return pltpu.make_async_remote_copy(
            src_ref=sums.at[source], dst_ref=sums.at[source], send_sem=tp_send.at[d], recv_sem=tp_recv.at[source],
            device_id={"tp": target}, device_id_type=MESH,
        )

    for d in range(1, columns):
        share(d, tp, lax.rem(tp + d, columns)).start()
    for d in range(1, columns):
        share(d, lax.rem(tp + d, columns), tp).wait_recv()
    everything = sums[0]
    for p in range(1, columns):
        everything = everything + sums[p]
    total[...] = everything

    if chips > 3:
        @pl.loop(3, chips)
        def _(s):
            for m in (0, 1):
                relay(s, m)

    for m in (0, 1):
        for p in range(chips):
            across(m, p, 1 - c).wait_recv()
            across(m, p, c).wait_send()

        @pl.loop(0, chips)
        def _(s):
            for k, sign in ((0, 1), (1, -1)):
                b = z - sign * s
                target = z + sign

                @pl.when((b >= 0) & (b < chips) & (target >= 0) & (target < chips))
                def _():
                    along(m, b, k, s, target * CORES + c).wait_send()

    for d in range(1, chips):
        scatter(d, z, lax.rem(z + d, chips)).wait_send()
        spread(d, z, lax.rem(z + d, chips)).wait_send()
    for p in range(chips):
        hand(p, c).wait_send()
    for d in range(1, columns):
        share(d, tp, lax.rem(tp + d, columns)).wait_send()


def communicate(fs, columns, x, qc, ho, oc, bq, bo, wq, wo):
    chips = fs // CORES
    tokens, width = x.shape
    features = qc.shape[1]
    rank = bq.shape[1]
    piece = rank // chips
    tile = 256 if tokens % 256 == 0 else tokens
    dma = pltpu.SemaphoreType.DMA
    f32 = jnp.float32
    return pl.pallas_call(
        functools.partial(exchange, chips, columns, tile),
        out_shape=(
            jax.ShapeDtypeStruct((fs,) + wq.shape, jnp.bfloat16),
            jax.ShapeDtypeStruct((fs,) + wo.shape, jnp.bfloat16),
            jax.ShapeDtypeStruct((CORES, chips, piece, features), f32),
            jax.ShapeDtypeStruct((8, 128), f32),
        ),
        in_specs=[pl.BlockSpec(memory_space=pltpu.HBM)] * 8,
        out_specs=[pl.BlockSpec(memory_space=pltpu.VMEM)] * 4,
        scratch_shapes=[
            pltpu.VMEM(x.shape, x.dtype),
            pltpu.VMEM(qc.shape, qc.dtype),
            pltpu.VMEM(ho.shape, ho.dtype),
            pltpu.VMEM(oc.shape, oc.dtype),
            pltpu.VMEM(bq.shape, bq.dtype),
            pltpu.VMEM(bo.shape, bo.dtype),
            pltpu.VMEM(wq.shape, wq.dtype),
            pltpu.VMEM(wo.shape, wo.dtype),
            pltpu.VMEM((2, rank, features), f32),
            pltpu.VMEM((rank, features), f32),
            pltpu.VMEM((chips, piece, features), f32),
            pltpu.VMEM((chips, piece, features), f32),
            pltpu.VMEM((columns, 8, 128), f32),
            dma((4, tokens // tile)),
            dma((4,)),
            dma((2, 2, chips)),
            dma((2, chips)),
            dma((2, chips)),
            dma((2, chips)),
            dma((2,)),
            dma((chips,)),
            dma((chips,)),
            dma((chips,)),
            dma((chips,)),
            dma((chips,)),
            dma((chips,)),
            dma((columns,)),
            dma((columns,)),
        ],
        compiler_params=pltpu.CompilerParams(
            collective_id=0, has_side_effects=True, vmem_limit_bytes=63 * 1024 * 1024
        ),
        name="exchange",
    )(x, qc, ho, oc, bq, bo, wq, wo)


def adam(low, first, second, factor):
    scaled = factor * low
    moment = BETA_FIRST * first + (1.0 - BETA_FIRST) * scaled
    square = BETA_SECOND * second + (1.0 - BETA_SECOND) * (scaled * scaled)
    return moment, square, moment / (jnp.sqrt(square) + ADAM_EPS)


def finish(fs, count, *refs):
    gq, go, low, total, bq, bo, wq, wo, fq, sq, fo, so = refs[:12]
    outs, made, sem = refs[12:22], refs[22:32], refs[32]
    step_q, step_o, new_q, new_o, copy_q, copy_o, moment_q, square_q, moment_o, square_o = made
    f32 = jnp.float32
    me = lax.axis_index("fs")
    rows = wq.shape[0]
    features = wo.shape[0]
    started = []

    def write(i, part=None, index=0):
        source, target = made[i], outs[i]
        if part is not None:
            source, target = source.at[part], target.at[part]
        copy = pltpu.make_async_copy(source, target, sem.at[i, index])
        copy.start()
        started.append(copy)

    factor = jnp.minimum(1.0, CLIP_RMS / jnp.sqrt(total[0:1, 0:1] * (1.0 / count) + NORM_EPS))
    low_q = jnp.concatenate([low[0, p] for p in range(low.shape[1])], axis=0)
    moment_q[...], square_q[...], dir_q = adam(low_q, fq[...], sq[...], factor)
    write(6)
    write(7)
    low_o = jnp.concatenate([low[1, p] for p in range(low.shape[1])], axis=0).T
    moment_o[...], square_o[...], dir_o = adam(low_o, fo[...], so[...], factor)
    write(8)
    write(9)
    pair_q = jnp.concatenate(split(dir_q), axis=0)
    pair_o = jnp.concatenate(split(dir_o), axis=1)

    def make_q(part):
        basis = bq[part, :]
        return jnp.dot(jnp.concatenate([basis, basis], axis=1), pair_q, preferred_element_type=f32)

    def make_o(left, part):
        basis = bo[part, :]
        both = jnp.concatenate([basis, basis], axis=1)
        return lax.dot_general(left, both, (((1,), (1,)), ((), ())), preferred_element_type=f32)

    mine = pl.ds(pl.multiple_of(me * rows, rows), rows)
    step = make_q(mine)
    step_q[...] = step
    new_q[...] = wq[...] - LEARN_RATE * step
    write(0)
    write(2)
    step = make_o(pair_o, mine)
    step_o[...] = step
    new_o[...] = wo[...] - LEARN_RATE * step
    write(1)
    write(3)

    for j in range(fs):
        part = pl.ds(j * rows, rows)
        copy_q[part, :] = (decode(gq[j]) - LEARN_RATE * make_q(part)).astype(copy_q.dtype)
        write(4, part, j)
    tall = 128
    for r in range(features // tall):
        part = pl.ds(r * tall, tall)
        left = pair_o[r * tall : (r + 1) * tall]
        for j in range(fs):
            columns = pl.ds(j * rows, rows)
            value = decode(go[j, part, :]) - LEARN_RATE * make_o(left, columns)
            copy_o[part, columns] = value.astype(copy_o.dtype)
        write(5, part, r)
    for copy in started:
        copy.wait()


def update(fs, columns, gq, go, low, total, bq, bo, wq, wo, fq, sq, fo, so):
    f32 = jnp.float32
    rank, features = fq.shape
    rows = wq.shape[0]
    width = fs * rows
    outs = (
        (wq.shape, f32), (wo.shape, f32), (wq.shape, f32), (wo.shape, f32),
        ((width, features), jnp.bfloat16), ((features, width), jnp.bfloat16),
        (fq.shape, f32), (fq.shape, f32), (fo.shape, f32), (fo.shape, f32),
    )
    return pl.pallas_call(
        functools.partial(finish, fs, 2 * rank * features * columns),
        out_shape=tuple(jax.ShapeDtypeStruct(*out) for out in outs),
        in_specs=[pl.BlockSpec(memory_space=pltpu.VMEM)] * 12,
        out_specs=[pl.BlockSpec(memory_space=pl.ANY)] * 10,
        scratch_shapes=[pltpu.VMEM(*out) for out in outs] + [pltpu.SemaphoreType.DMA((10, max(fs, features // 128)))],
        compiler_params=pltpu.CompilerParams(vmem_limit_bytes=63 * 1024 * 1024),
        name="update",
    )(gq, go, low, total, bq, bo, wq, wo, fq, sq, fo, so)


def shards(
    fs, columns,
    saved_input, query_cot, head_out, output_cot, basis_q, basis_o,
    weight_q, weight_o, first_q, second_q, first_o, second_o,
):
    all_q, all_o, low, total = communicate(
        fs, columns, saved_input, query_cot, head_out, output_cot, basis_q, basis_o, weight_q, weight_o
    )
    return update(
        fs, columns, all_q, all_o, low, total, basis_q, basis_o,
        weight_q, weight_o, first_q, second_q, first_o, second_o,
    )


def solution(mesh):
    return jax.shard_map(
        functools.partial(shards, mesh.shape["fs"], mesh.shape["tp"]),
        mesh=mesh,
        in_specs=(
            P("fs", None), P("fs", "tp"), P("fs", "tp"), P("fs", None), P(), P(),
            P("fs", "tp"), P("tp", "fs"), P(None, "tp"), P(None, "tp"), P("tp", None), P("tp", None),
        ),
        out_specs=(
            P("fs", "tp"), P("tp", "fs"), P("fs", "tp"), P("tp", "fs"), P(None, "tp"), P("tp", None),
            P(None, "tp"), P(None, "tp"), P("tp", None), P("tp", None),
        ),
        check_vma=False,
    )
```
